32 devices in a mesh: grp: 2 (over y), ep: 4 (over z), tp: 4 (over x, core).
Axes of the slice: x: 2, y: 2, z: 4, core: 2. Of those that a mesh axis runs over, the one named last changes fastest.
Arguments:
- tokens: bfloat16 [80, 1024], P(('grp', 'ep')), parts along dimension 0, may hold values from -40 to 40
- attn_gain: float32 [1024], replicated, may hold values from 0.1 to 1.9
- w_query: bfloat16 [1024, 1024], P(None, 'tp'), may hold values from -0.1875 to 0.1875
- w_key: bfloat16 [1024, 512], P(None, 'tp'), may hold values from -0.1875 to 0.1875
- w_value: bfloat16 [1024, 512], P(None, 'tp'), may hold values from -0.1875 to 0.1875
- key_cache: bfloat16 [80, 512, 1024], P(('grp', 'ep'), 'tp'), parts along dimension 0, may hold values from -6 to 6
- value_cache: bfloat16 [80, 512, 1024], P(('grp', 'ep'), 'tp'), parts along dimension 0, may hold values from -6 to 6
- lengths: int32 [80], P(('grp', 'ep')), parts along dimension 0, may hold values from 256 to 1024
- head_bias: float32 [16], P('tp'), may hold values from -8 to -2
- w_out: bfloat16 [1024, 1024], P(None, 'tp'), may hold values from -0.1875 to 0.1875
- ffn_gain: float32 [1024], replicated, may hold values from 0.1 to 1.9
- route_ids: int32 [80, 2], P(('grp', 'ep')), parts along dimension 0, may hold values from 0 to 3, all different within a row; in each aligned block of 10 rows (0 to 9, 10 to 19, ...) at most 10 rows name the same one
- route_weights: float32 [80, 2], P(('grp', 'ep')), parts along dimension 0, may hold values from 0.1 to 1
- w_gate: bfloat16 [4, 1024, 2048], P('ep', None, 'tp'), may hold values from -0.1875 to 0.1875
- w_up: bfloat16 [4, 1024, 2048], P('ep', None, 'tp'), may hold values from -0.1875 to 0.1875
- w_down: bfloat16 [4, 2048, 1024], P('ep', 'tp'), may hold values from -0.125 to 0.125
Outputs:
- mixed: bfloat16 [80, 1024], P(('grp', 'ep'), 'tp'), parts along dimension 0
- new_keys: bfloat16 [80, 512], P(('grp', 'ep'), 'tp'), parts along dimension 0
- new_values: bfloat16 [80, 512], P(('grp', 'ep'), 'tp'), parts along dimension 0
The draws below stay inside these ranges and needn't reach their ends.
There are 2 independent parts, one for each index of `grp`. The reference program is written for one: setup_inputs(seed, part) draws one part's arguments, and reference() takes and returns one part's arrays. A program takes and returns all parts, laid end to end along the dimension named above; an argument that names none is the same for every part. Nothing has to cross between parts.
Inputs may be any that keep to these rules, and one draw needn't show every extreme that they name: `route_ids`: each row names 2 different experts. In each aligned block of 10 rows no expert is named more than 10 times, and in some block some expert is named exactly 10 times.
All inputs are finite; a program needn't handle non-finite values.
Results may differ from the reference program's by a relative error of at most 0.012.
Values may be sent and summed in bfloat16 or wider, within the bound.
A program may use at most 64 MiB of HBM per device.

```python
import math
import jax
import jax.numpy as jnp
import numpy as np
from jax import lax

D = 1024
HEADS = 16
KV_HEADS = 8
HEAD_SIZE = 64
FF = 2048
TOPK = 2
SEQ_DEV = 10
CACHE_LEN = 1024
QDIM = 1024
KVDIM = 512
SEQS = 40
EXPERTS = 4
CAP = 10
N_EP = 4
N_TP = 4


def draw_tokens(key, part):
    base_key = jax.random.fold_in(key, 11)
    key_rows, key_cols, key_base = jax.random.split(base_key, 3)
    row_scale = jnp.exp(jax.random.uniform(key_rows, (SEQS, 1), jnp.float32, math.log(0.3), math.log(3.0)))
    position = jnp.arange(D, dtype=jnp.float32) / D - 0.5
    rough = jnp.exp(jax.random.uniform(key_cols, (1, D), jnp.float32, -0.35, 0.35))
    col_scale = jnp.exp(math.log(3.0) * position)[None, :] * rough
    base = jnp.clip(jax.random.normal(key_base, (SEQS, D), jnp.float32), -5.0, 5.0)
    return (base * row_scale * col_scale).astype(jnp.bfloat16)


def place_ends(drawn, stream_key, smallest, largest):
    index_at = [jax.random.randint(jax.random.fold_in(stream_key, axis), (), 0, length) for axis, length in enumerate(drawn.shape)]
    longest = drawn.shape.index(max(drawn.shape))
    beside = index_at[:longest] + [(index_at[longest] + 1) % drawn.shape[longest]] + index_at[longest + 1:]
    return drawn.at[tuple(index_at)].set(smallest).at[tuple(beside)].set(largest)


def level_of(own_key, shape, cuts, smallest, largest):
    def one(dim, parts):
        steps = jax.random.uniform(jax.random.fold_in(jax.random.fold_in(own_key, 6), dim), (parts,), jnp.float32, smallest / len(cuts), largest / len(cuts))
        return jnp.repeat(jnp.exp(steps), shape[dim] // parts).reshape((-1,) + (1,) * (len(shape) - dim - 1))

    level = one(*cuts[0])
    for cut in cuts[1:]:
        level = level * one(*cut)
    return level


def assign_block(own_key, own, number, rows, amount, top, limit, skew):
    sequence = jax.random.permutation(own_key, amount)
    heavy_load, usual = shares(amount, rows * top, limit, skew, True), shares(amount, rows * top, limit, skew, False)
    places = jnp.arange(amount)

    def named(sizes, rotation):
        used = int((sizes > 0).sum())
        fixed = max(1, used // 4)
        passed = fixed + (places - fixed + rotation * (used - fixed)) % max(1, amount - fixed)
        return jnp.zeros((amount,), jnp.int32).at[sequence[jnp.where(places < fixed, places, passed)]].set(jnp.asarray(sizes, jnp.int32))

    sizes = jnp.where(number % 4 == 0, named(heavy_load, number // 4), named(usual, number - number // 4 - 1))
    mixed = jax.random.permutation(jax.random.fold_in(own, 3), amount)
    source_of, receiver = mixed[0:amount // 2 * 2:2], mixed[1:amount // 2 * 2:2]
    room = jnp.minimum(sizes[source_of] - 1, limit - sizes[receiver]) // 2
    room = jnp.where((source_of == sequence[0]) | (receiver == sequence[0]) | (sizes[receiver] == 0), 0, jnp.maximum(room, 0))
    passed = jax.random.randint(jax.random.fold_in(own, 4), (amount // 2,), 0, 1 << 20) % (room + 1)
    sizes = sizes.at[source_of].add(-passed).at[receiver].add(passed)
    members = jnp.searchsorted(jnp.cumsum(sizes), jnp.arange(rows * top), side="right").astype(jnp.int32)
    grid = members.reshape(top, rows).T
    grid = grid[jax.random.permutation(jax.random.fold_in(own, 1), rows)]
    rotation = jax.random.randint(jax.random.fold_in(own, 2), (rows, 1), 0, top)
    return jnp.take_along_axis(grid, (jnp.arange(top)[None, :] + rotation) % top, axis=1)


def shares(number_of, total, reach, slope, full):
    loads = [(1 << 20) // math.isqrt(grade ** slope) + 1 for grade in range(1, number_of + 1)]
    largest = reach if full else min(reach, max(-(-total // number_of), total * loads[0] // sum(loads)))
    least = 1 if total - largest >= number_of - 1 else 0
    counts, surplus = [largest] + [least] * (number_of - 1), total - largest - least * (number_of - 1)
    while surplus > 0:
        candidates = [i for i in range(1, number_of) if counts[i] < largest] or [i for i in range(1, number_of) if counts[i] < reach]
        pool, budget = sum([loads[i] for i in candidates]), surplus
        for i in candidates:
            extra = min(reach - counts[i], max(1, budget * loads[i] // pool), surplus)
            counts[i] = counts[i] + extra
            surplus = surplus - extra
    return np.array(counts)


def scatter_about(rng, extent, spread, limit, shards=(), kind=jnp.bfloat16):
    level = level_of(rng, extent, shards, -0.22, 0.18) if shards else 1.0
    entries = jax.random.normal(rng, extent, jnp.float32) * spread * level
    return jnp.minimum(jnp.maximum(entries, -limit), limit).astype(kind)


def setup_inputs(seed: int = 0, part: int = 0) -> dict:
    keys = jax.random.split(jax.random.key(seed), 17)
    own_keys = jax.random.split(jax.random.fold_in(keys[16], part), 17)
    tokens = draw_tokens(jax.random.fold_in(jax.random.fold_in(keys[16], part), 71), part)
    attn_gain = jnp.clip(1.0 + 0.18 * jax.random.normal(keys[1], (D,), jnp.float32), 0.1, 1.9)
    w_query = scatter_about(keys[2], (D, QDIM), D ** -0.5, 0.1875, ((1, 4),))
    w_key = scatter_about(keys[3], (D, KVDIM), D ** -0.5, 0.1875, ((1, 4),))
    w_value = scatter_about(keys[4], (D, KVDIM), D ** -0.5, 0.1875, ((1, 4),))
    key_cache = scatter_about(own_keys[5], (SEQS, KVDIM, CACHE_LEN), 1.0, 6.0, ((0, 4), (1, 4)))
    value_cache = scatter_about(own_keys[6], (SEQS, KVDIM, CACHE_LEN), 1.0, 6.0, ((0, 4), (1, 4)))
    lengths = place_ends(jax.random.randint(own_keys[7], (SEQS,), CACHE_LEN // 4, CACHE_LEN + 1), jax.random.fold_in(own_keys[7], 1), CACHE_LEN // 4, CACHE_LEN).astype(jnp.int32)
    head_bias = jnp.clip(-8.0 + 6.0 * jax.random.uniform(keys[8], (HEADS,), jnp.float32) ** level_of(keys[8], (HEADS,), ((0, 4),), -0.2, 0.2), -8.0, -2.0)
    w_out = scatter_about(keys[9], (QDIM, D), QDIM ** -0.5, 0.1875, ((1, 4),))
    ffn_gain = jnp.clip(1.0 + 0.18 * jax.random.normal(keys[10], (D,), jnp.float32), 0.1, 1.9)
    route_ids_keys = jax.random.split(jax.random.fold_in(own_keys[11], 1), SEQS // SEQ_DEV)
    route_ids_turns = jax.random.permutation(jax.random.fold_in(own_keys[11], 3), SEQS // SEQ_DEV)
    route_ids = jax.vmap(lambda own, number: assign_block(jax.random.fold_in(own_keys[11], 2), own, number, SEQ_DEV, EXPERTS, TOPK, CAP, 2))(route_ids_keys, route_ids_turns).reshape((SEQS, TOPK))
    route_weights = jnp.clip(0.1 + 0.9 * jax.random.uniform(own_keys[12], (SEQS, TOPK), jnp.float32) ** level_of(own_keys[12], (SEQS, TOPK), ((0, 4),), -0.2, 0.2), 0.1, 1.0)
    w_gate = scatter_about(keys[13], (EXPERTS, D, FF), D ** -0.5, 0.1875, ((0, 4), (2, 4)))
    w_up = scatter_about(keys[14], (EXPERTS, D, FF), D ** -0.5, 0.1875, ((0, 4), (2, 4)))
    w_down = scatter_about(keys[15], (EXPERTS, FF, D), FF ** -0.5, 0.125, ((0, 4), (1, 4)))
    return {"tokens": tokens, "attn_gain": attn_gain, "w_query": w_query, "w_key": w_key, "w_value": w_value, "key_cache": key_cache, "value_cache": value_cache, "lengths": lengths, "head_bias": head_bias, "w_out": w_out, "ffn_gain": ffn_gain, "route_ids": route_ids, "route_weights": route_weights, "w_gate": w_gate, "w_up": w_up, "w_down": w_down}


epsilon = 1e-06

def rms_rows(values, gain):
    mean_sq = lax.optimization_barrier(jnp.mean(values * values, axis=-1, keepdims=True))
    return values * lax.rsqrt(mean_sq + epsilon) * gain

def attend_one(queries, key_block, value_block, length, head_shift):
    group_size = HEADS // KV_HEADS
    query_heads = queries.astype(jnp.float32).reshape(KV_HEADS, group_size, HEAD_SIZE)
    key_heads = key_block.astype(jnp.float32).reshape(KV_HEADS, HEAD_SIZE, CACHE_LEN)
    value_heads = value_block.astype(jnp.float32).reshape(KV_HEADS, HEAD_SIZE, CACHE_LEN)
    scores = jnp.einsum('kgd,kdl->kgl', query_heads, key_heads) * HEAD_SIZE ** (-0.5)
    scores = scores + head_shift.reshape(KV_HEADS, group_size)[:, :, None]
    in_cache = jnp.arange(CACHE_LEN, dtype=jnp.int32)[None, None, :] < length
    log_rest = jnp.where(in_cache, jax.nn.log_sigmoid(-scores), 0.0)
    tail_sum = lax.cumsum(log_rest, axis=2, reverse=True) - log_rest
    breaks = jnp.where(in_cache, jnp.exp(jax.nn.log_sigmoid(scores) + tail_sum), 0.0).astype(jnp.bfloat16)
    heads_out = jnp.einsum('kgl,kdl->kgd', breaks.astype(jnp.float32), value_heads)
    return heads_out.reshape(QDIM).astype(jnp.bfloat16)

def reference(tokens, attn_gain, w_query, w_key, w_value, key_cache, value_cache, lengths, head_bias, w_out, ffn_gain, route_ids, route_weights, w_gate, w_up, w_down):
    token_rows = tokens.astype(jnp.float32)
    normed = rms_rows(token_rows, attn_gain).astype(jnp.bfloat16)
    queries = jnp.dot(normed, w_query, preferred_element_type=jnp.float32).astype(jnp.bfloat16)
    new_keys = jnp.dot(normed, w_key, preferred_element_type=jnp.float32).astype(jnp.bfloat16)
    new_values = jnp.dot(normed, w_value, preferred_element_type=jnp.float32).astype(jnp.bfloat16)

    def per_sequence(items):
        return attend_one(items[0], items[1], items[2], items[3], head_bias)
    heads_out = lax.map(per_sequence, (queries, key_cache, value_cache, lengths))
    attn_out = jnp.dot(heads_out, w_out, preferred_element_type=jnp.float32)
    hidden = token_rows + attn_out
    ffn_in = rms_rows(hidden, ffn_gain).astype(jnp.bfloat16)
    pair_expert = route_ids.reshape(-1)
    pair_weight = route_weights.reshape(-1)
    most_rows = N_EP * CAP

    def one_expert(running, expert):
        matches = pair_expert == expert
        pair_order = jnp.argsort(jnp.where(matches, 0, 1).astype(jnp.int32), stable=True)[:most_rows]
        is_live = matches[pair_order]
        token_index = (pair_order // TOPK).astype(jnp.int32)
        chosen = jnp.where(is_live[:, None], ffn_in[token_index], jnp.zeros((), jnp.bfloat16))
        gate_act = jnp.dot(chosen, w_gate[expert], preferred_element_type=jnp.float32)
        up_act = jnp.dot(chosen, w_up[expert], preferred_element_type=jnp.float32)
        hidden_act = (jax.nn.silu(gate_act) * up_act).astype(jnp.bfloat16)
        inner_groups = hidden_act.astype(jnp.float32).reshape(most_rows, N_TP, FF // N_TP)
        down_groups = w_down[expert].astype(jnp.float32).reshape(N_TP, FF // N_TP, D)
        group_terms = jnp.einsum('rgf,gfd->rgd', inner_groups, down_groups).astype(jnp.bfloat16)
        result = lax.optimization_barrier(jnp.sum(group_terms.astype(jnp.float32), axis=1)).astype(jnp.bfloat16)
        pair_scale = jnp.where(is_live, pair_weight[pair_order], 0.0)
        running = running.at[token_index].add(result.astype(jnp.float32) * pair_scale[:, None])
        return (running, None)
    routed_sum, _ = lax.scan(one_expert, jnp.zeros((SEQS, D), jnp.float32), jnp.arange(EXPERTS, dtype=jnp.int32))
    mixed = (hidden + routed_sum).astype(jnp.bfloat16)
    return (mixed, new_keys, new_values)
```

```python
import functools

import jax
import jax.numpy as jnp
from jax import lax
from jax.experimental import pallas as pl
from jax.experimental.pallas import tpu as pltpu
from jax.sharding import PartitionSpec as P

HEAD_SIZE = 64
EPSILON = 1e-06
ROW_TILE = 16
MESH_IDS = pl.DeviceIdType.MESH
F32 = jnp.float32
BF16 = jnp.bfloat16


def iota(shape, dim):
    return lax.broadcasted_iota(jnp.int32, shape, dim)


def dot(a, b):
    return jnp.dot(a, b, preferred_element_type=F32)


def layer_kernel(
    n_ep,
    n_tp,
    tokens_hbm,
    attn_gain_hbm,
    w_query_hbm,
    w_key_hbm,
    w_value_hbm,
    key_hbm,
    value_hbm,
    lengths_hbm,
    head_bias_hbm,
    w_out_hbm,
    ffn_gain_hbm,
    route_ids_hbm,
    route_weights_hbm,
    w_gate_hbm,
    w_up_hbm,
    w_down_hbm,
    mixed_ref,
    new_keys_ref,
    new_values_ref,
    tokens,
    attn_gain,
    w_query,
    w_key,
    w_value,
    keys,
    values,
    lengths,
    head_bias,
    w_out,
    ffn_gain,
    route_ids,
    route_weights,
    w_gate,
    w_up,
    w_down,
    spread,
    head_part,
    head_all,
    hidden_part,
    hidden_all,
    ffn_rows,
    out_parts,
    returned,
    small_sem,
    pair_sem,
    weight_sem,
    send_sem,
    recv_sem,
):
    ep = lax.axis_index("ep")
    tp = lax.axis_index("tp")
    me = ep * n_tp + tp
    n_peers = n_ep * n_tp
    rows = tokens.shape[0]
    query_cols = w_query.shape[1]
    key_cols = w_key_hbm.shape[1]
    heads = query_cols // HEAD_SIZE
    group = query_cols // key_cols
    slice_width = w_out.shape[1]
    cache_len = keys.shape[2]
    pairs = rows // 2

    def far_ep(step):
        from_top = jnp.where(n_ep - 1 - step > ep, n_ep - 1 - step, n_ep - 2 - step)
        from_bottom = jnp.where(step < ep, step, step + 1)
        return jnp.where(2 * ep < n_ep, from_top, from_bottom)

    def other_tp(step):
        chip = lax.rem(tp // 2 + 1 + step // 2, n_tp // 2)
        return chip * 2 + lax.rem(tp + step, 2)

    tp_order = [other_tp(step) for step in range(n_tp - 2)]
    tp_order += [other_tp(n_tp - 1), tp]

    def each_peer(fn):
        def to_ep(step):
            for peer_tp in tp_order:
                fn(far_ep(step), peer_tp)

        if n_peers <= 16:
            for step in range(n_ep - 1):
                to_ep(step)
        else:
            pl.loop(0, n_ep - 1)(to_ep)
        for peer_tp in tp_order[:-1]:
            fn(ep, peer_tp)

    barrier = pltpu.get_barrier_semaphore()

    def greet(peer_ep, peer_tp):
        pl.semaphore_signal(
            barrier,
            inc=1,
            device_id={"ep": peer_ep, "tp": peer_tp},
            device_id_type=MESH_IDS,
        )

    def load(source, target, sem):
        copy = pltpu.make_async_copy(source, target, sem)
        copy.start()
        return copy

    token_load = load(tokens_hbm, tokens, small_sem.at[0])
    gain_load = load(attn_gain_hbm, attn_gain, small_sem.at[1])
    query_load = load(w_query_hbm, w_query, small_sem.at[2])
    cache_loads = []
    for number, (source, target) in enumerate(((key_hbm, keys), (value_hbm, values))):
        for half in reversed(range(2)):
            part = pl.ds(half * (cache_len // 2), cache_len // 2)
            for third in range(2):
                seqs = pl.ds(third * pairs, pairs)
                pltpu.make_async_copy(
                    source.at[seqs, :, part],
                    target.at[seqs, :, part],
                    pair_sem.at[2 * number + 1 - half],
                ).start()
            whole = target.at[:, :, part]
            cache_loads.append(
                pltpu.make_async_copy(whole, whole, pair_sem.at[2 * number + 1 - half])
            )
        if number == 0:
            for step in range(n_ep - 1):
                greet(far_ep(step), tp)
            for peer_tp in tp_order[:-1]:
                greet(ep, peer_tp)
            length_load = load(lengths_hbm, lengths, small_sem.at[3])
            bias_load = load(head_bias_hbm, head_bias, small_sem.at[4])
    own_loads = [
        load(w_key_hbm, w_key, small_sem.at[5]),
        load(w_value_hbm, w_value, small_sem.at[9]),
    ]
    out_load = load(w_out_hbm, w_out, weight_sem.at[0])
    route_loads = [
        load(ffn_gain_hbm, ffn_gain, small_sem.at[6]),
        load(route_ids_hbm, route_ids, small_sem.at[7]),
        load(route_weights_hbm, route_weights, small_sem.at[8]),
    ]
    weight_loads = [
        load(w_gate_hbm, w_gate, weight_sem.at[1]),
        load(w_up_hbm, w_up, weight_sem.at[2]),
        load(w_down_hbm, w_down, weight_sem.at[3]),
    ]
    ffn_rows[...] = jnp.zeros_like(ffn_rows)

    block_len = 256 if cache_len % 256 == 0 else 128
    n_blocks = cache_len // block_len
    triangle = (
        iota((block_len, block_len), 0) > iota((block_len, block_len), 1)
    ).astype(BF16)
    flat = rows * heads
    seq_col = lax.rem(iota((flat, 1), 0), rows)
    head_col = iota((flat, 1), 0) // rows

    token_load.wait()
    rows_f32 = tokens[...].astype(F32)
    gain_load.wait()
    normed = (
        rows_f32
        * lax.rsqrt(jnp.mean(rows_f32 * rows_f32, axis=1, keepdims=True) + EPSILON)
        * attn_gain[...]
    ).astype(BF16)
    query_load.wait()
    queries = dot(normed, w_query[...]).astype(BF16).astype(F32)
    for head in range(heads):
        first = head // group * HEAD_SIZE
        piece = queries[:, head * HEAD_SIZE : (head + 1) * HEAD_SIZE]
        sides = [jnp.zeros((rows, first), F32)] if first else []
        sides.append(piece)
        if key_cols > first + HEAD_SIZE:
            sides.append(jnp.zeros((rows, key_cols - first - HEAD_SIZE), F32))
        spread[head * rows : (head + 1) * rows, :] = jnp.concatenate(sides, axis=1)
    folded = spread[...].astype(BF16)
    query_block = jnp.where(
        iota((flat, rows * key_cols), 1) // key_cols == seq_col,
        jnp.concatenate([folded] * rows, axis=1),
        0.0,
    ).astype(BF16)

    length_load.wait()
    bias_load.wait()
    length_col = jnp.zeros((flat, 1), jnp.int32)
    for row in range(rows):
        length_col = jnp.where(seq_col == row, lengths[row], length_col)
    bias_col = jnp.zeros((flat, 1), F32)
    for head in range(heads):
        bias_col = jnp.where(head_col == head, head_bias[head], bias_col)

    for copy in cache_loads[:2]:
        copy.wait()
    key_rows = keys[...].reshape(rows * key_cols, cache_len)
    scores = dot(query_block, key_rows) * HEAD_SIZE ** (-0.5) + bias_col
    in_cache = iota((flat, cache_len), 1) < length_col
    soft = jnp.log(1.0 + jnp.exp(-jnp.abs(scores)))
    log_rest = jnp.where(in_cache, jnp.minimum(-scores, 0.0) - soft, 0.0)
    log_take = jnp.minimum(scores, 0.0) - soft
    high = log_rest.astype(BF16)
    low = (log_rest - high.astype(F32)).astype(BF16)
    stacked = jnp.concatenate(
        [
            part[:, block * block_len : (block + 1) * block_len]
            for part in (high, low)
            for block in range(n_blocks)
        ],
        axis=0,
    )
    within = dot(stacked, triangle)
    carried = jnp.zeros((flat, 1), F32)
    tails = [None] * n_blocks
    for block in reversed(range(n_blocks)):
        tails[block] = (
            within[block * flat : (block + 1) * flat]
            + within[(n_blocks + block) * flat : (n_blocks + block + 1) * flat]
            + carried
        )
        part = log_rest[:, block * block_len : (block + 1) * block_len]
        carried = carried + jnp.sum(part, axis=1, keepdims=True)
    tail_sum = jnp.concatenate(tails, axis=1)
    breaks = jnp.where(in_cache, jnp.exp(log_take + tail_sum), 0.0).astype(BF16)
    for copy in cache_loads[2:]:
        copy.wait()
    value_rows = values[...].reshape(rows * key_cols, cache_len)
    crossed = lax.dot_general(
        breaks, value_rows, (((1,), (1,)), ((), ())), preferred_element_type=F32
    )
    own = jnp.zeros((flat, key_cols), F32)
    for row in range(rows):
        own = jnp.where(seq_col == row, crossed[:, row * key_cols : (row + 1) * key_cols], own)
    spread[...] = own
    heads_out = jnp.concatenate(
        [
            spread[
                head * rows : (head + 1) * rows,
                head // group * HEAD_SIZE : (head // group + 1) * HEAD_SIZE,
            ]
            for head in range(heads)
        ],
        axis=1,
    ).astype(BF16)

    pl.semaphore_wait(barrier, n_ep + n_tp - 2)
    head_part[...] = heads_out
    own_cols = pl.ds(pl.multiple_of(tp * query_cols, query_cols), query_cols)
    head_slot = head_all.at[:, own_cols]
    for peer_tp in tp_order[:-1]:
        pltpu.make_async_remote_copy(
            src_ref=head_part,
            dst_ref=head_slot,
            send_sem=send_sem.at[0],
            recv_sem=recv_sem.at[0],
            device_id={"tp": peer_tp},
            device_id_type=MESH_IDS,
        ).start()
    pltpu.make_async_copy(head_part, head_slot, recv_sem.at[0]).start()
    for copy in own_loads:
        copy.wait()
    new_keys_ref[...] = dot(normed, w_key[...]).astype(BF16)
    new_values_ref[...] = dot(normed, w_value[...]).astype(BF16)
    out_load.wait()
    pltpu.make_async_copy(head_all, head_all, recv_sem.at[0]).wait()
    attn_out = dot(head_all[...], w_out[...])

    slice_cols = pl.ds(pl.multiple_of(tp * slice_width, slice_width), slice_width)
    own_hidden = tokens[:, slice_cols].astype(F32) + attn_out
    hidden_part[...] = own_hidden.astype(BF16)
    hidden_slot = hidden_all.at[ep, :, slice_cols]

    def send_hidden(peer_ep, peer_tp):
        pltpu.make_async_remote_copy(
            src_ref=hidden_part,
            dst_ref=hidden_slot,
            send_sem=send_sem.at[1],
            recv_sem=recv_sem.at[1],
            device_id={"ep": peer_ep, "tp": peer_tp},
            device_id_type=MESH_IDS,
        ).start()

    each_peer(send_hidden)
    pltpu.make_async_copy(hidden_part, hidden_slot, recv_sem.at[1]).start()
    for copy in route_loads:
        copy.wait()
    diagonal = iota((rows, rows), 0) == iota((rows, rows), 1)
    choices = []
    for choice in range(route_ids.shape[0]):
        id_row = route_ids[choice : choice + 1, :].astype(F32)
        weight_row = route_weights[choice : choice + 1, :]
        choices.append(
            tuple(
                jnp.sum(jnp.where(diagonal, row, 0.0), axis=1, keepdims=True)
                for row in (id_row, weight_row)
            )
        )
    for copy in weight_loads:
        copy.wait()
    pltpu.make_async_copy(hidden_all, hidden_all, recv_sem.at[1]).wait()
    for source in range(n_ep):
        hidden = hidden_all[source].astype(F32)
        first = source * ROW_TILE
        ffn_rows[first : first + rows, :] = (
            hidden
            * lax.rsqrt(jnp.mean(hidden * hidden, axis=1, keepdims=True) + EPSILON)
            * ffn_gain[...]
        ).astype(BF16)
    ffn_in = ffn_rows[...]

    gate_act = dot(ffn_in, w_gate[0])
    up_act = dot(ffn_in, w_up[0])
    hidden_act = (gate_act / (1.0 + jnp.exp(-gate_act)) * up_act).astype(BF16)
    for step in range(n_tp):
        to_tp = tp_order[step]
        part = pl.ds(pl.multiple_of(to_tp * slice_width, slice_width), slice_width)
        partial_out = dot(hidden_act, w_down[0, :, part]).astype(BF16)
        for owner in range(n_ep):
            first = owner * ROW_TILE
            out_parts[step, owner] = partial_out[first : first + rows]

        def send_out(to_ep):
            pltpu.make_async_remote_copy(
                src_ref=out_parts.at[step, to_ep],
                dst_ref=returned.at[me],
                send_sem=send_sem.at[2],
                recv_sem=recv_sem.at[2],
                device_id={"ep": to_ep, "tp": to_tp},
                device_id_type=MESH_IDS,
            ).start()

        if n_ep <= 8:
            for hop in range(n_ep - 1):
                send_out(far_ep(hop))
        else:

            @pl.loop(0, n_ep - 1)
            def _(hop):
                send_out(far_ep(hop))

        if step < n_tp - 1:
            send_out(ep)
        else:
            pltpu.make_async_copy(
                out_parts.at[step, ep],
                returned.at[me],
                recv_sem.at[2],
            ).start()
    pltpu.make_async_copy(returned, returned, recv_sem.at[2]).wait()
    mixed = own_hidden
    for expert in range(n_ep):
        total = returned[expert * n_tp].astype(F32)
        for number in range(1, n_tp):
            total = total + returned[expert * n_tp + number].astype(F32)
        scale = jnp.zeros((rows, 1), F32)
        for id_col, weight_col in choices:
            scale = scale + jnp.where(id_col == expert, weight_col, 0.0)
        mixed = mixed + scale * total.astype(BF16).astype(F32)
    mixed_ref[...] = mixed.astype(BF16)

    sent = head_all.at[:, pl.ds(0, (n_tp - 1) * query_cols)]
    pltpu.make_async_copy(sent, sent, send_sem.at[0]).wait()
    sent = returned.at[pl.ds(0, n_peers - 1)]
    pltpu.make_async_copy(sent, sent, send_sem.at[1]).wait()
    pltpu.make_async_copy(sent, sent, send_sem.at[2]).wait()


def place_results(*refs):
    copies = [
        pltpu.make_async_copy(refs[number], refs[3 + number], refs[6].at[number])
        for number in range(3)
    ]
    for copy in copies:
        copy.start()
    for copy in copies:
        copy.wait()


def shards(
    tokens,
    attn_gain,
    w_query,
    w_key,
    w_value,
    key_cache,
    value_cache,
    lengths,
    head_bias,
    w_out,
    ffn_gain,
    route_ids,
    route_weights,
    w_gate,
    w_up,
    w_down,
):
    n_ep = lax.axis_size("ep")
    n_tp = lax.axis_size("tp")
    rows, width = tokens.shape
    query_cols = w_query.shape[1]
    key_cols = w_key.shape[1]
    slice_width = w_out.shape[1]
    operands = (
        tokens,
        attn_gain.reshape(1, width),
        w_query,
        w_key,
        w_value,
        key_cache,
        value_cache,
        lengths,
        head_bias,
        w_out,
        ffn_gain.reshape(1, width),
        route_ids.T,
        route_weights.T,
        w_gate,
        w_up,
        w_down,
    )
    in_smem = (7, 8)
    buffers = [
        (pltpu.SMEM if number in in_smem else pltpu.VMEM)(operand.shape, operand.dtype)
        for number, operand in enumerate(operands)
    ]
    n_peers = n_ep * n_tp
    scratch = buffers + [
        pltpu.VMEM((rows * (query_cols // HEAD_SIZE), key_cols), F32),
        pltpu.VMEM((rows, query_cols), BF16),
        pltpu.VMEM((rows, query_cols * n_tp), BF16),
        pltpu.VMEM((rows, slice_width), BF16),
        pltpu.VMEM((n_ep, rows, width), BF16),
        pltpu.VMEM((n_ep * ROW_TILE, width), BF16),
        pltpu.VMEM((n_tp, n_ep, rows, slice_width), BF16),
        pltpu.VMEM((n_peers, rows, slice_width), BF16),
        pltpu.SemaphoreType.DMA((10,)),
        pltpu.SemaphoreType.DMA((4,)),
        pltpu.SemaphoreType.DMA((4,)),
        pltpu.SemaphoreType.DMA((3,)),
        pltpu.SemaphoreType.DMA((3,)),
    ]
    results = pl.pallas_call(
        functools.partial(layer_kernel, n_ep, n_tp),
        out_shape=(
            pltpu.VMEM((rows, slice_width), BF16),
            pltpu.VMEM((rows, key_cols), BF16),
            pltpu.VMEM((rows, key_cols), BF16),
        ),
        in_specs=[pl.BlockSpec(memory_space=pltpu.HBM)] * len(operands),
        out_specs=tuple([pl.BlockSpec(memory_space=pltpu.VMEM)] * 3),
        scratch_shapes=scratch,
        compiler_params=pltpu.CompilerParams(
            collective_id=0, has_side_effects=True, vmem_limit_bytes=66990080
        ),
        name="layer",
    )(*operands)
    return pl.pallas_call(
        place_results,
        out_shape=tuple(jax.ShapeDtypeStruct(r.shape, r.dtype) for r in results),
        in_specs=[pl.BlockSpec(memory_space=pltpu.VMEM)] * 3,
        out_specs=tuple([pl.BlockSpec(memory_space=pltpu.HBM)] * 3),
        scratch_shapes=[pltpu.SemaphoreType.DMA((3,))],
        compiler_params=pltpu.CompilerParams(vmem_limit_bytes=2**20),
        name="place",
    )(*results)


def solution(mesh):
    in_specs = (
        P(("grp", "ep"), None),
        P(),
        P(None, "tp"),
        P(None, "tp"),
        P(None, "tp"),
        P(("grp", "ep"), "tp", None),
        P(("grp", "ep"), "tp", None),
        P(("grp", "ep")),
        P("tp"),
        P(None, "tp"),
        P(),
        P(("grp", "ep"), None),
        P(("grp", "ep"), None),
        P("ep", None, "tp"),
        P("ep", None, "tp"),
        P("ep", "tp", None),
    )
    out_specs = (P(("grp", "ep"), "tp"), P(("grp", "ep"), "tp"), P(("grp", "ep"), "tp"))
    return jax.shard_map(shards, mesh=mesh, in_specs=in_specs, out_specs=out_specs, check_vma=False)
```

```python
import functools

import jax
import jax.numpy as jnp
from jax import lax
from jax.experimental import pallas as pl
from jax.experimental.pallas import tpu as pltpu
from jax.sharding import PartitionSpec as P

HEAD_SIZE = 64
EPSILON = 1e-06
ROW_TILE = 16
MESH_IDS = pl.DeviceIdType.MESH
F32 = jnp.float32
BF16 = jnp.bfloat16


def iota(shape, dim):
    return lax.broadcasted_iota(jnp.int32, shape, dim)


def dot(a, b):
    return jnp.dot(a, b, preferred_element_type=F32)


def layer_kernel(
    n_ep,
    n_tp,
    n_messages,
    tokens_hbm,
    attn_gain_hbm,
    w_query_hbm,
    w_key_hbm,
    w_value_hbm,
    key_hbm,
    value_hbm,
    lengths_hbm,
    head_bias_hbm,
    w_out_hbm,
    ffn_gain_hbm,
    route_ids_hbm,
    route_weights_hbm,
    w_gate_hbm,
    w_up_hbm,
    w_down_hbm,
    mixed_ref,
    new_keys_ref,
    new_values_ref,
    tokens,
    attn_gain,
    w_query,
    w_key,
    w_value,
    keys,
    values,
    lengths,
    head_bias,
    w_out,
    ffn_gain,
    route_ids,
    route_weights,
    w_in,
    w_down,
    spread,
    head_part,
    head_all,
    hidden_part,
    hidden_all,
    hidden_rows,
    out_parts,
    returned,
    small_sem,
    pair_sem,
    weight_sem,
    send_sem,
    recv_sem,
):
    ep = lax.axis_index("ep")
    tp = lax.axis_index("tp")
    rows = tokens.shape[0]
    query_cols = w_query.shape[1]
    key_cols = w_key_hbm.shape[1]
    heads = query_cols // HEAD_SIZE
    group = query_cols // key_cols
    slice_width = w_out.shape[1]
    cache_len = keys.shape[2]
    pairs = rows // 2

    def far_ep(step):
        from_top = jnp.where(n_ep - 1 - step > ep, n_ep - 1 - step, n_ep - 2 - step)
        from_bottom = jnp.where(step < ep, step, step + 1)
        return jnp.where(2 * ep < n_ep, from_top, from_bottom)

    def other_tp(step):
        chip = lax.rem(tp // 2 + 1 + step // 2, n_tp // 2)
        return chip * 2 + lax.rem(tp + step, 2)

    tp_order = [other_tp(step) for step in range(n_tp - 2)]
    tp_order += [other_tp(n_tp - 1), tp]

    share = n_ep * n_tp // n_messages
    half, chips = n_ep // share, n_tp // share
    side, chip, keeper = lax.rem(tp, share), tp // share, ep // half
    first_ep = side * half
    mine = keeper == side
    other_chips = [lax.rem(chip + 1 + step, chips) for step in range(chips - 1)]

    def copy_to(source, target, number, peer_ep, peer_tp):
        pltpu.make_async_remote_copy(
            src_ref=source,
            dst_ref=target,
            send_sem=send_sem.at[number],
            recv_sem=recv_sem.at[number],
            device_id={"ep": peer_ep, "tp": peer_tp},
            device_id_type=MESH_IDS,
        ).start()

    def repeat(count, fn):
        if count <= 4:
            for step in range(count):
                fn(step)
        else:
            pl.loop(0, count)(fn)

    barrier = pltpu.get_barrier_semaphore()

    def greet(peer_ep, peer_tp):
        pl.semaphore_signal(
            barrier,
            inc=1,
            device_id={"ep": peer_ep, "tp": peer_tp},
            device_id_type=MESH_IDS,
        )

    def load(source, target, sem):
        copy = pltpu.make_async_copy(source, target, sem)
        copy.start()
        return copy

    token_load = load(tokens_hbm, tokens, small_sem.at[0])
    gain_load = load(attn_gain_hbm, attn_gain, small_sem.at[1])
    query_load = load(w_query_hbm, w_query, small_sem.at[2])
    cache_loads = []
    for number, (source, target) in enumerate(((key_hbm, keys), (value_hbm, values))):
        for upper in reversed(range(2)):
            part = pl.ds(upper * (cache_len // 2), cache_len // 2)
            for third in range(2):
                seqs = pl.ds(third * pairs, pairs)
                pltpu.make_async_copy(
                    source.at[seqs, :, part],
                    target.at[seqs, :, part],
                    pair_sem.at[2 * number + 1 - upper],
                ).start()
            whole = target.at[:, :, part]
            cache_loads.append(
                pltpu.make_async_copy(whole, whole, pair_sem.at[2 * number + 1 - upper])
            )
        if number == 0:
            for step in range(n_ep - 1):
                greet(far_ep(step), tp)
            for peer_tp in tp_order[:-1]:
                greet(ep, peer_tp)
            length_load = load(lengths_hbm, lengths, small_sem.at[3])
            bias_load = load(head_bias_hbm, head_bias, small_sem.at[4])
    own_loads = [
        load(w_key_hbm, w_key, small_sem.at[5]),
        load(w_value_hbm, w_value, small_sem.at[9]),
    ]
    out_load = load(w_out_hbm, w_out, weight_sem.at[0])
    route_loads = [
        load(ffn_gain_hbm, ffn_gain, small_sem.at[6]),
        load(route_ids_hbm, route_ids, small_sem.at[7]),
        load(route_weights_hbm, route_weights, small_sem.at[8]),
    ]
    weight_loads = [
        load(w_gate_hbm.at[0], w_in.at[0, 0], weight_sem.at[1]),
        load(w_up_hbm.at[0], w_in.at[0, 1], weight_sem.at[2]),
        load(w_down_hbm.at[0], w_down.at[0], weight_sem.at[3]),
    ]
    hidden_rows[...] = jnp.zeros_like(hidden_rows)

    block_len = 256 if cache_len % 256 == 0 else 128
    n_blocks = cache_len // block_len
    triangle = (
        iota((block_len, block_len), 0) > iota((block_len, block_len), 1)
    ).astype(BF16)
    flat = rows * heads
    seq_col = lax.rem(iota((flat, 1), 0), rows)
    head_col = iota((flat, 1), 0) // rows

    token_load.wait()
    rows_f32 = tokens[...].astype(F32)
    gain_load.wait()
    normed = (
        rows_f32
        * lax.rsqrt(jnp.mean(rows_f32 * rows_f32, axis=1, keepdims=True) + EPSILON)
        * attn_gain[...]
    ).astype(BF16)
    query_load.wait()
    queries = dot(normed, w_query[...]).astype(BF16).astype(F32)
    for head in range(heads):
        first = head // group * HEAD_SIZE
        piece = queries[:, head * HEAD_SIZE : (head + 1) * HEAD_SIZE]
        sides = [jnp.zeros((rows, first), F32)] if first else []
        sides.append(piece)
        if key_cols > first + HEAD_SIZE:
            sides.append(jnp.zeros((rows, key_cols - first - HEAD_SIZE), F32))
        spread[head * rows : (head + 1) * rows, :] = jnp.concatenate(sides, axis=1)
    folded = spread[...].astype(BF16)
    query_block = jnp.where(
        iota((flat, rows * key_cols), 1) // key_cols == seq_col,
        jnp.concatenate([folded] * rows, axis=1),
        0.0,
    ).astype(BF16)

    length_load.wait()
    bias_load.wait()
    length_col = jnp.zeros((flat, 1), jnp.int32)
    for row in range(rows):
        length_col = jnp.where(seq_col == row, lengths[row], length_col)
    bias_col = jnp.zeros((flat, 1), F32)
    for head in range(heads):
        bias_col = jnp.where(head_col == head, head_bias[head], bias_col)

    for copy in cache_loads[:2]:
        copy.wait()
    key_rows = keys[...].reshape(rows * key_cols, cache_len)
    scores = dot(query_block, key_rows) * HEAD_SIZE ** (-0.5) + bias_col
    in_cache = iota((flat, cache_len), 1) < length_col
    soft = jnp.log(1.0 + jnp.exp(-jnp.abs(scores)))
    log_rest = jnp.where(in_cache, jnp.minimum(-scores, 0.0) - soft, 0.0)
    log_take = jnp.minimum(scores, 0.0) - soft
    high = log_rest.astype(BF16)
    low = (log_rest - high.astype(F32)).astype(BF16)
    stacked = jnp.concatenate(
        [
            part[:, block * block_len : (block + 1) * block_len]
            for part in (high, low)
            for block in range(n_blocks)
        ],
        axis=0,
    )
    within = dot(stacked, triangle)
    carried = jnp.zeros((flat, 1), F32)
    tails = [None] * n_blocks
    for block in reversed(range(n_blocks)):
        tails[block] = (
            within[block * flat : (block + 1) * flat]
            + within[(n_blocks + block) * flat : (n_blocks + block + 1) * flat]
            + carried
        )
        part = log_rest[:, block * block_len : (block + 1) * block_len]
        carried = carried + jnp.sum(part, axis=1, keepdims=True)
    tail_sum = jnp.concatenate(tails, axis=1)
    breaks = jnp.where(in_cache, jnp.exp(log_take + tail_sum), 0.0).astype(BF16)
    for copy in cache_loads[2:]:
        copy.wait()
    value_rows = values[...].reshape(rows * key_cols, cache_len)
    crossed = lax.dot_general(
        breaks, value_rows, (((1,), (1,)), ((), ())), preferred_element_type=F32
    )
    own = jnp.zeros((flat, key_cols), F32)
    for row in range(rows):
        own = jnp.where(seq_col == row, crossed[:, row * key_cols : (row + 1) * key_cols], own)
    spread[...] = own
    heads_out = jnp.concatenate(
        [
            spread[
                head * rows : (head + 1) * rows,
                head // group * HEAD_SIZE : (head // group + 1) * HEAD_SIZE,
            ]
            for head in range(heads)
        ],
        axis=1,
    ).astype(BF16)

    pl.semaphore_wait(barrier, n_ep + n_tp - 2)
    head_part[...] = heads_out
    own_cols = pl.ds(pl.multiple_of(tp * query_cols, query_cols), query_cols)
    head_slot = head_all.at[:, own_cols]
    for peer_tp in tp_order[:-1]:
        copy_to(head_part, head_slot, 0, ep, peer_tp)
    pltpu.make_async_copy(head_part, head_slot, recv_sem.at[0]).start()
    partner = tp + 1 - 2 * side
    for copy in weight_loads:
        copy.wait()
    if share == 2:
        copy_to(w_in.at[0], w_in.at[1], 3, ep, partner)
    for copy in own_loads:
        copy.wait()
    new_keys_ref[...] = dot(normed, w_key[...]).astype(BF16)
    new_values_ref[...] = dot(normed, w_value[...]).astype(BF16)
    out_load.wait()
    pltpu.make_async_copy(head_all, head_all, recv_sem.at[0]).wait()
    attn_out = dot(head_all[...], w_out[...])

    slice_cols = pl.ds(pl.multiple_of(tp * slice_width, slice_width), slice_width)
    own_hidden = tokens[:, slice_cols].astype(F32) + attn_out
    rounded = own_hidden.astype(BF16)
    for pair in range(pairs):
        hidden_part[pair] = rounded[2 * pair : 2 * pair + 2]
    hidden_slot = hidden_all.at[lax.rem(ep, half), tp]

    def send_hidden(step):
        for peer_chip in other_chips + [chip]:
            copy_to(hidden_part, hidden_slot, 1, far_ep(step), peer_chip * share + keeper)

    repeat(n_ep - 1, send_hidden)
    for peer_chip in other_chips:
        copy_to(hidden_part, hidden_slot, 1, ep, peer_chip * share + keeper)

    @pl.when(mine)
    def _():
        pltpu.make_async_copy(hidden_part, hidden_slot, recv_sem.at[1]).start()

    if share == 2:

        @pl.when(jnp.logical_not(mine))
        def _():
            copy_to(hidden_part, hidden_slot, 1, ep, partner)

        copy_to(w_down.at[0], w_down.at[1], 4, ep, partner)
    for copy in route_loads:
        copy.wait()
    diagonal = iota((rows, rows), 0) == iota((rows, rows), 1)
    choices = []
    for choice in range(route_ids.shape[0]):
        id_row = route_ids[choice : choice + 1, :].astype(F32)
        weight_row = route_weights[choice : choice + 1, :]
        choices.append(
            tuple(
                jnp.sum(jnp.where(diagonal, row, 0.0), axis=1, keepdims=True)
                for row in (id_row, weight_row)
            )
        )
    if share == 2:
        pltpu.make_async_copy(w_in.at[1], w_in.at[1], recv_sem.at[3]).wait()
    pltpu.make_async_copy(hidden_all, hidden_all, recv_sem.at[1]).wait()
    for source in range(half):
        for peer_tp in range(n_tp):
            part = slice(peer_tp * slice_width, (peer_tp + 1) * slice_width)
            for pair in range(pairs):
                first = source * ROW_TILE + 2 * pair
                hidden_rows[first : first + 2, part] = hidden_all[
                    source, peer_tp, pair
                ].astype(F32)
    hidden = hidden_rows[...]
    scaled = (hidden * ffn_gain[...]).astype(BF16)
    row_scale = lax.rsqrt(jnp.mean(hidden * hidden, axis=1, keepdims=True) + EPSILON)
    acts = []
    for member in range(share):
        gate_act = dot(scaled, w_in[member, 0]) * row_scale
        up_act = dot(scaled, w_in[member, 1]) * row_scale
        acts.append((gate_act / (1.0 + jnp.exp(-gate_act)) * up_act).astype(BF16))
    hidden_act = jnp.concatenate(acts, axis=1)
    if share == 2:
        pltpu.make_async_copy(w_down.at[1], w_down.at[1], recv_sem.at[4]).wait()
    expert_rows = dot(hidden_act, w_down[...].reshape(hidden_act.shape[1], -1)).astype(BF16)
    for source in range(half):
        for peer_tp in range(n_tp):
            part = slice(peer_tp * slice_width, (peer_tp + 1) * slice_width)
            for pair in range(pairs):
                first = source * ROW_TILE + 2 * pair
                out_parts[peer_tp, source, pair] = expert_rows[first : first + 2, part]
    out_slot = returned.at[ep * chips + chip]

    def far_owner(step):
        return jnp.where(2 * ep >= 2 * first_ep + half, step, half - 1 - step)

    def send_out(step):
        source = far_owner(step)
        for peer_tp in tp_order[:-1]:
            copy_to(out_parts.at[peer_tp, source], out_slot, 2, first_ep + source, peer_tp)

    def send_own(step):
        source = far_owner(step)

        @pl.when(first_ep + source != ep)
        def _():
            copy_to(out_parts.at[tp, source], out_slot, 2, first_ep + source, tp)

        @pl.when(first_ep + source == ep)
        def _():
            pltpu.make_async_copy(out_parts.at[tp, source], out_slot, recv_sem.at[2]).start()

    repeat(half, send_out)
    repeat(half, send_own)
    pltpu.make_async_copy(returned, returned, recv_sem.at[2]).wait()

    def expert_part(number):
        return jnp.concatenate(
            [returned[number, pair].astype(F32) for pair in range(pairs)], axis=0
        )

    mixed = own_hidden
    for expert in range(n_ep):
        total = expert_part(expert * chips)
        for number in range(1, chips):
            total = total + expert_part(expert * chips + number)
        scale = jnp.zeros((rows, 1), F32)
        for id_col, weight_col in choices:
            scale = scale + jnp.where(id_col == expert, weight_col, 0.0)
        mixed = mixed + scale * total.astype(BF16).astype(F32)
    mixed_ref[...] = mixed.astype(BF16)

    sent = head_all.at[:, pl.ds(0, (n_tp - 1) * query_cols)]
    pltpu.make_async_copy(sent, sent, send_sem.at[0]).wait()
    for number in (1, 2):

        @pl.when(mine)
        def _():
            sent = returned.at[pl.ds(0, n_messages - 1)]
            pltpu.make_async_copy(sent, sent, send_sem.at[number]).wait()

        @pl.when(jnp.logical_not(mine))
        def _():
            pltpu.make_async_copy(returned, returned, send_sem.at[number]).wait()

    if share == 2:
        pltpu.make_async_copy(w_in.at[1], w_in.at[1], send_sem.at[3]).wait()
        pltpu.make_async_copy(w_down.at[1], w_down.at[1], send_sem.at[4]).wait()


def place_results(*refs):
    copies = [
        pltpu.make_async_copy(refs[number], refs[3 + number], refs[6].at[number])
        for number in range(3)
    ]
    for copy in copies:
        copy.start()
    for copy in copies:
        copy.wait()


def shards(
    tokens,
    attn_gain,
    w_query,
    w_key,
    w_value,
    key_cache,
    value_cache,
    lengths,
    head_bias,
    w_out,
    ffn_gain,
    route_ids,
    route_weights,
    w_gate,
    w_up,
    w_down,
):
    n_ep = lax.axis_size("ep")
    n_tp = lax.axis_size("tp")
    rows, width = tokens.shape
    query_cols = w_query.shape[1]
    key_cols = w_key.shape[1]
    slice_width = w_out.shape[1]
    operands = (
        tokens,
        attn_gain.reshape(1, width),
        w_query,
        w_key,
        w_value,
        key_cache,
        value_cache,
        lengths,
        head_bias,
        w_out,
        ffn_gain.reshape(1, width),
        route_ids.T,
        route_weights.T,
        w_gate,
        w_up,
        w_down,
    )
    in_smem = (7, 8)
    buffers = [
        (pltpu.SMEM if number in in_smem else pltpu.VMEM)(operand.shape, operand.dtype)
        for number, operand in enumerate(operands[:13])
    ]
    share = 2 if n_ep % 2 == 0 and n_tp % 2 == 0 else 1
    half, pairs = n_ep // share, rows // 2
    n_messages = half * n_tp
    hidden_units = w_gate.shape[2]
    scratch = buffers + [
        pltpu.VMEM((share, 2, width, hidden_units), BF16),
        pltpu.VMEM((share, hidden_units, width), BF16),
        pltpu.VMEM((rows * (query_cols // HEAD_SIZE), key_cols), F32),
        pltpu.VMEM((rows, query_cols), BF16),
        pltpu.VMEM((rows, query_cols * n_tp), BF16),
        pltpu.VMEM((pairs, 2, slice_width), BF16),
        pltpu.VMEM((half, n_tp, pairs, 2, slice_width), BF16),
        pltpu.VMEM((half * ROW_TILE, width), F32),
        pltpu.VMEM((n_tp, half, pairs, 2, slice_width), BF16),
        pltpu.VMEM((n_messages, pairs, 2, slice_width), BF16),
        pltpu.SemaphoreType.DMA((10,)),
        pltpu.SemaphoreType.DMA((4,)),
        pltpu.SemaphoreType.DMA((4,)),
        pltpu.SemaphoreType.DMA((5,)),
        pltpu.SemaphoreType.DMA((5,)),
    ]
    results = pl.pallas_call(
        functools.partial(layer_kernel, n_ep, n_tp, n_messages),
        out_shape=(
            pltpu.VMEM((rows, slice_width), BF16),
            pltpu.VMEM((rows, key_cols), BF16),
            pltpu.VMEM((rows, key_cols), BF16),
        ),
        in_specs=[pl.BlockSpec(memory_space=pltpu.HBM)] * len(operands),
        out_specs=tuple([pl.BlockSpec(memory_space=pltpu.VMEM)] * 3),
        scratch_shapes=scratch,
        compiler_params=pltpu.CompilerParams(
            collective_id=0, has_side_effects=True, vmem_limit_bytes=66990080
        ),
        name="layer",
    )(*operands)
    return pl.pallas_call(
        place_results,
        out_shape=tuple(jax.ShapeDtypeStruct(r.shape, r.dtype) for r in results),
        in_specs=[pl.BlockSpec(memory_space=pltpu.VMEM)] * 3,
        out_specs=tuple([pl.BlockSpec(memory_space=pltpu.HBM)] * 3),
        scratch_shapes=[pltpu.SemaphoreType.DMA((3,))],
        compiler_params=pltpu.CompilerParams(vmem_limit_bytes=2**20),
        name="place",
    )(*results)


def solution(mesh):
    in_specs = (
        P(("grp", "ep"), None),
        P(),
        P(None, "tp"),
        P(None, "tp"),
        P(None, "tp"),
        P(("grp", "ep"), "tp", None),
        P(("grp", "ep"), "tp", None),
        P(("grp", "ep")),
        P("tp"),
        P(None, "tp"),
        P(),
        P(("grp", "ep"), None),
        P(("grp", "ep"), None),
        P("ep", None, "tp"),
        P("ep", None, "tp"),
        P("ep", "tp", None),
    )
    out_specs = (P(("grp", "ep"), "tp"), P(("grp", "ep"), "tp"), P(("grp", "ep"), "tp"))
    return jax.shard_map(shards, mesh=mesh, in_specs=in_specs, out_specs=out_specs, check_vma=False)
```

```python
import functools

import jax
import jax.numpy as jnp
from jax import lax
from jax.experimental import pallas as pl
from jax.experimental.pallas import tpu as pltpu
from jax.sharding import PartitionSpec as P

HEAD_SIZE = 64
EPSILON = 1e-06
ROW_TILE = 16
MESH_IDS = pl.DeviceIdType.MESH
F32 = jnp.float32
BF16 = jnp.bfloat16


def iota(shape, dim):
    return lax.broadcasted_iota(jnp.int32, shape, dim)


def dot(a, b):
    return jnp.dot(a, b, preferred_element_type=F32)


def layer_kernel(
    n_ep,
    n_tp,
    n_messages,
    tokens_hbm,
    attn_gain_hbm,
    w_query_hbm,
    w_key_hbm,
    w_value_hbm,
    key_hbm,
    value_hbm,
    lengths_hbm,
    head_bias_hbm,
    w_out_hbm,
    ffn_gain_hbm,
    route_ids_hbm,
    route_weights_hbm,
    w_gate_hbm,
    w_up_hbm,
    w_down_hbm,
    mixed_ref,
    new_keys_ref,
    new_values_ref,
    tokens,
    attn_gain,
    w_query,
    w_key,
    w_value,
    keys,
    values,
    lengths,
    head_bias,
    w_out,
    ffn_gain,
    route_ids,
    route_weights,
    w_in,
    w_down,
    spread,
    head_part,
    head_all,
    hidden_part,
    hidden_all,
    hidden_rows,
    out_parts,
    returned,
    small_sem,
    pair_sem,
    weight_sem,
    send_sem,
    recv_sem,
):
    ep = lax.axis_index("ep")
    tp = lax.axis_index("tp")
    rows = tokens.shape[0]
    query_cols = w_query.shape[1]
    key_cols = w_key_hbm.shape[1]
    heads = query_cols // HEAD_SIZE
    group = query_cols // key_cols
    slice_width = w_out.shape[1]
    cache_len = keys.shape[2]
    pairs = rows // 2

    def far_ep(step):
        from_top = jnp.where(n_ep - 1 - step > ep, n_ep - 1 - step, n_ep - 2 - step)
        from_bottom = jnp.where(step < ep, step, step + 1)
        return jnp.where(2 * ep < n_ep, from_top, from_bottom)

    def other_tp(step):
        chip = lax.rem(tp // 2 + 1 + step // 2, n_tp // 2)
        return chip * 2 + lax.rem(tp + step, 2)

    tp_order = [other_tp(step) for step in range(n_tp - 2)]
    tp_order += [other_tp(n_tp - 1), tp]

    share = n_ep * n_tp // n_messages
    half, chips = n_ep // share, n_tp // share
    side, chip, keeper = lax.rem(tp, share), tp // share, share - 1 - ep // half
    first_ep = (share - 1 - side) * half
    mine = keeper == side
    other_chips = [lax.rem(chip + 1 + step, chips) for step in range(chips - 1)]

    def copy_to(source, target, number, peer_ep, peer_tp):
        pltpu.make_async_remote_copy(
            src_ref=source,
            dst_ref=target,
            send_sem=send_sem.at[number],
            recv_sem=recv_sem.at[number],
            device_id={"ep": peer_ep, "tp": peer_tp},
            device_id_type=MESH_IDS,
        ).start()

    def repeat(count, fn):
        if count <= 4:
            for step in range(count):
                fn(step)
        else:
            pl.loop(0, count)(fn)

    barrier = pltpu.get_barrier_semaphore()

    def greet(peer_ep, peer_tp):
        pl.semaphore_signal(
            barrier,
            inc=1,
            device_id={"ep": peer_ep, "tp": peer_tp},
            device_id_type=MESH_IDS,
        )

    def load(source, target, sem):
        copy = pltpu.make_async_copy(source, target, sem)
        copy.start()
        return copy

    token_load = load(tokens_hbm, tokens, small_sem.at[0])
    gain_load = load(attn_gain_hbm, attn_gain, small_sem.at[1])
    query_load = load(w_query_hbm, w_query, small_sem.at[2])
    def load_cache(source, target, sem):
        for pair in range(pairs):
            part = pl.ds(2 * pair, 2)
            pltpu.make_async_copy(source.at[part], target.at[part], sem).start()
        return pltpu.make_async_copy(target, target, sem)

    key_load = load_cache(key_hbm, keys, pair_sem.at[0])
    for step in range(n_ep - 1):
        greet(far_ep(step), tp)
    for peer_tp in tp_order[:-1]:
        greet(ep, peer_tp)
    value_load = load_cache(value_hbm, values, pair_sem.at[1])
    length_load = load(lengths_hbm, lengths, small_sem.at[3])
    bias_load = load(head_bias_hbm, head_bias, small_sem.at[4])
    hidden_rows[...] = jnp.zeros_like(hidden_rows)

    block_len = 256 if cache_len % 256 == 0 else 128
    n_blocks = cache_len // block_len
    triangle = (
        iota((block_len, block_len), 0) > iota((block_len, block_len), 1)
    ).astype(BF16)
    flat = rows * heads
    seq_col = lax.rem(iota((flat, 1), 0), rows)
    head_col = iota((flat, 1), 0) // rows

    token_load.wait()
    rows_f32 = tokens[...].astype(F32)
    gain_load.wait()
    normed = (
        rows_f32
        * lax.rsqrt(jnp.mean(rows_f32 * rows_f32, axis=1, keepdims=True) + EPSILON)
        * attn_gain[...]
    ).astype(BF16)
    query_load.wait()
    own_loads = [
        load(w_key_hbm, w_key, small_sem.at[5]),
        load(w_value_hbm, w_value, small_sem.at[9]),
    ]
    out_load = load(w_out_hbm, w_out, weight_sem.at[0])
    route_loads = [
        load(ffn_gain_hbm, ffn_gain, small_sem.at[6]),
        load(route_ids_hbm, route_ids, small_sem.at[7]),
        load(route_weights_hbm, route_weights, small_sem.at[8]),
    ]
    for number, source in enumerate((w_gate_hbm, w_up_hbm)):
        pltpu.make_async_copy(source.at[0], w_in.at[0, number], weight_sem.at[1]).start()
    weight_loads = [
        pltpu.make_async_copy(w_in.at[0], w_in.at[0], weight_sem.at[1]),
        load(w_down_hbm.at[0], w_down.at[0], weight_sem.at[2]),
    ]
    queries = dot(normed, w_query[...]).astype(BF16).astype(F32)
    for head in range(heads):
        first = head // group * HEAD_SIZE
        piece = queries[:, head * HEAD_SIZE : (head + 1) * HEAD_SIZE]
        sides = [jnp.zeros((rows, first), F32)] if first else []
        sides.append(piece)
        if key_cols > first + HEAD_SIZE:
            sides.append(jnp.zeros((rows, key_cols - first - HEAD_SIZE), F32))
        spread[head * rows : (head + 1) * rows, :] = jnp.concatenate(sides, axis=1)
    folded = spread[...].astype(BF16)
    query_block = jnp.where(
        iota((flat, rows * key_cols), 1) // key_cols == seq_col,
        jnp.concatenate([folded] * rows, axis=1),
        0.0,
    ).astype(BF16)

    length_load.wait()
    bias_load.wait()
    length_col = jnp.zeros((flat, 1), jnp.int32)
    for row in range(rows):
        length_col = jnp.where(seq_col == row, lengths[row], length_col)
    bias_col = jnp.zeros((flat, 1), F32)
    for head in range(heads):
        bias_col = jnp.where(head_col == head, head_bias[head], bias_col)

    key_load.wait()
    key_rows = keys[...].reshape(rows * key_cols, cache_len)
    scores = dot(query_block, key_rows) * HEAD_SIZE ** (-0.5) + bias_col
    in_cache = iota((flat, cache_len), 1) < length_col
    soft = jnp.log(1.0 + jnp.exp(-jnp.abs(scores)))
    log_rest = jnp.where(in_cache, jnp.minimum(-scores, 0.0) - soft, 0.0)
    log_take = jnp.minimum(scores, 0.0) - soft
    high = log_rest.astype(BF16)
    low = (log_rest - high.astype(F32)).astype(BF16)
    stacked = jnp.concatenate(
        [
            part[:, block * block_len : (block + 1) * block_len]
            for part in (high, low)
            for block in range(n_blocks)
        ],
        axis=0,
    )
    within = dot(stacked, triangle)
    carried = jnp.zeros((flat, 1), F32)
    tails = [None] * n_blocks
    for block in reversed(range(n_blocks)):
        tails[block] = (
            within[block * flat : (block + 1) * flat]
            + within[(n_blocks + block) * flat : (n_blocks + block + 1) * flat]
            + carried
        )
        part = log_rest[:, block * block_len : (block + 1) * block_len]
        carried = carried + jnp.sum(part, axis=1, keepdims=True)
    tail_sum = jnp.concatenate(tails, axis=1)
    breaks = jnp.where(in_cache, jnp.exp(log_take + tail_sum), 0.0).astype(BF16)
    value_load.wait()
    value_rows = values[...].reshape(rows * key_cols, cache_len)
    crossed = lax.dot_general(
        breaks, value_rows, (((1,), (1,)), ((), ())), preferred_element_type=F32
    )
    own = jnp.zeros((flat, key_cols), F32)
    for row in range(rows):
        own = jnp.where(seq_col == row, crossed[:, row * key_cols : (row + 1) * key_cols], own)
    spread[...] = own
    heads_out = jnp.concatenate(
        [
            spread[
                head * rows : (head + 1) * rows,
                head // group * HEAD_SIZE : (head // group + 1) * HEAD_SIZE,
            ]
            for head in range(heads)
        ],
        axis=1,
    ).astype(BF16)

    pl.semaphore_wait(barrier, n_ep + n_tp - 2)
    head_part[...] = heads_out
    own_cols = pl.ds(pl.multiple_of(tp * query_cols, query_cols), query_cols)
    head_slot = head_all.at[:, own_cols]
    for peer_tp in tp_order[:-1]:
        copy_to(head_part, head_slot, 0, ep, peer_tp)
    pltpu.make_async_copy(head_part, head_slot, recv_sem.at[0]).start()
    partner = tp + 1 - 2 * side
    for copy in weight_loads:
        copy.wait()
    if share == 2:
        copy_to(w_in.at[0], w_in.at[1], 3, ep, partner)
    for copy in own_loads:
        copy.wait()
    new_keys_ref[...] = dot(normed, w_key[...]).astype(BF16)
    new_values_ref[...] = dot(normed, w_value[...]).astype(BF16)
    out_load.wait()
    pltpu.make_async_copy(head_all, head_all, recv_sem.at[0]).wait()
    attn_out = dot(head_all[...], w_out[...])

    slice_cols = pl.ds(pl.multiple_of(tp * slice_width, slice_width), slice_width)
    own_hidden = tokens[:, slice_cols].astype(F32) + attn_out
    rounded = own_hidden.astype(BF16)
    for pair in range(pairs):
        hidden_part[pair] = rounded[2 * pair : 2 * pair + 2]
    hidden_slot = hidden_all.at[lax.rem(ep, half), tp]

    def send_hidden(step):
        for peer_chip in other_chips + [chip]:
            copy_to(hidden_part, hidden_slot, 1, far_ep(step), peer_chip * share + keeper)

    repeat(n_ep - 1, send_hidden)
    for peer_chip in other_chips:
        copy_to(hidden_part, hidden_slot, 1, ep, peer_chip * share + keeper)

    @pl.when(mine)
    def _():
        pltpu.make_async_copy(hidden_part, hidden_slot, recv_sem.at[1]).start()

    if share == 2:

        @pl.when(jnp.logical_not(mine))
        def _():
            copy_to(hidden_part, hidden_slot, 1, ep, partner)

        copy_to(w_down.at[0], w_down.at[1], 4, ep, partner)
    for copy in route_loads:
        copy.wait()
    diagonal = iota((rows, rows), 0) == iota((rows, rows), 1)
    choices = []
    for choice in range(route_ids.shape[0]):
        id_row = route_ids[choice : choice + 1, :].astype(F32)
        weight_row = route_weights[choice : choice + 1, :]
        choices.append(
            tuple(
                jnp.sum(jnp.where(diagonal, row, 0.0), axis=1, keepdims=True)
                for row in (id_row, weight_row)
            )
        )
    if share == 2:
        pltpu.make_async_copy(w_in.at[1], w_in.at[1], recv_sem.at[3]).wait()
    pltpu.make_async_copy(hidden_all, hidden_all, recv_sem.at[1]).wait()
    for source in range(half):
        for peer_tp in range(n_tp):
            part = slice(peer_tp * slice_width, (peer_tp + 1) * slice_width)
            for pair in range(pairs):
                first = source * ROW_TILE + 2 * pair
                hidden_rows[first : first + 2, part] = hidden_all[
                    source, peer_tp, pair
                ].astype(F32)
    hidden = hidden_rows[...]
    scaled = (hidden * ffn_gain[...]).astype(BF16)
    row_scale = lax.rsqrt(jnp.mean(hidden * hidden, axis=1, keepdims=True) + EPSILON)
    acts = []
    for member in range(share):
        gate_act = dot(scaled, w_in[member, 0]) * row_scale
        up_act = dot(scaled, w_in[member, 1]) * row_scale
        acts.append((gate_act / (1.0 + jnp.exp(-gate_act)) * up_act).astype(BF16))
    hidden_act = jnp.concatenate(acts, axis=1)
    if share == 2:
        pltpu.make_async_copy(w_down.at[1], w_down.at[1], recv_sem.at[4]).wait()
    out_slot = returned.at[ep * chips + chip]
    chip_width = share * slice_width
    for order, peer_chip in enumerate(other_chips + [chip]):
        cols = pl.ds(pl.multiple_of(peer_chip * chip_width, chip_width), chip_width)
        down = w_down[:, :, cols].reshape(hidden_act.shape[1], chip_width)
        expert_rows = dot(hidden_act, down).astype(BF16)
        for source in range(half):
            for member in range(share):
                part = slice(member * slice_width, (member + 1) * slice_width)
                for pair in range(pairs):
                    first = source * ROW_TILE + 2 * pair
                    out_parts[order, member, source, pair] = expert_rows[first : first + 2, part]

        def send_out(step):
            source = jnp.where(2 * ep >= 2 * first_ep + half, step, half - 1 - step)
            owner = first_ep + source
            if order < chips - 1:
                for member in range(share):
                    peer_tp = peer_chip * share + member
                    copy_to(out_parts.at[order, member, source], out_slot, 2, owner, peer_tp)
                return
            if share == 2:
                copy_to(out_parts.at[order, 1 - side, source], out_slot, 2, owner, partner)

            @pl.when(owner != ep)
            def _():
                copy_to(out_parts.at[order, side, source], out_slot, 2, owner, tp)

            @pl.when(owner == ep)
            def _():
                pltpu.make_async_copy(
                    out_parts.at[order, side, source], out_slot, recv_sem.at[2]
                ).start()

        repeat(half, send_out)
    pltpu.make_async_copy(returned, returned, recv_sem.at[2]).wait()

    def expert_part(number):
        return jnp.concatenate(
            [returned[number, pair].astype(F32) for pair in range(pairs)], axis=0
        )

    mixed = own_hidden
    for expert in range(n_ep):
        total = expert_part(expert * chips)
        for number in range(1, chips):
            total = total + expert_part(expert * chips + number)
        scale = jnp.zeros((rows, 1), F32)
        for id_col, weight_col in choices:
            scale = scale + jnp.where(id_col == expert, weight_col, 0.0)
        mixed = mixed + scale * total.astype(BF16).astype(F32)
    mixed_ref[...] = mixed.astype(BF16)

    sent = head_all.at[:, pl.ds(0, (n_tp - 1) * query_cols)]
    pltpu.make_async_copy(sent, sent, send_sem.at[0]).wait()
    for number in (1, 2):

        @pl.when(mine)
        def _():
            sent = returned.at[pl.ds(0, n_messages - 1)]
            pltpu.make_async_copy(sent, sent, send_sem.at[number]).wait()

        @pl.when(jnp.logical_not(mine))
        def _():
            pltpu.make_async_copy(returned, returned, send_sem.at[number]).wait()

    if share == 2:
        pltpu.make_async_copy(w_in.at[1], w_in.at[1], send_sem.at[3]).wait()
        pltpu.make_async_copy(w_down.at[1], w_down.at[1], send_sem.at[4]).wait()


def place_results(*refs):
    copies = [
        pltpu.make_async_copy(refs[number], refs[3 + number], refs[6].at[number])
        for number in range(3)
    ]
    for copy in copies:
        copy.start()
    for copy in copies:
        copy.wait()


def shards(
    tokens,
    attn_gain,
    w_query,
    w_key,
    w_value,
    key_cache,
    value_cache,
    lengths,
    head_bias,
    w_out,
    ffn_gain,
    route_ids,
    route_weights,
    w_gate,
    w_up,
    w_down,
):
    n_ep = lax.axis_size("ep")
    n_tp = lax.axis_size("tp")
    rows, width = tokens.shape
    query_cols = w_query.shape[1]
    key_cols = w_key.shape[1]
    slice_width = w_out.shape[1]
    operands = (
        tokens,
        attn_gain.reshape(1, width),
        w_query,
        w_key,
        w_value,
        key_cache,
        value_cache,
        lengths,
        head_bias,
        w_out,
        ffn_gain.reshape(1, width),
        route_ids.T,
        route_weights.T,
        w_gate,
        w_up,
        w_down,
    )
    in_smem = (7, 8)
    buffers = [
        (pltpu.SMEM if number in in_smem else pltpu.VMEM)(operand.shape, operand.dtype)
        for number, operand in enumerate(operands[:13])
    ]
    share = 2 if n_ep % 2 == 0 and n_tp % 2 == 0 else 1
    half, pairs = n_ep // share, rows // 2
    n_messages = half * n_tp
    hidden_units = w_gate.shape[2]
    scratch = buffers + [
        pltpu.VMEM((share, 2, width, hidden_units), BF16),
        pltpu.VMEM((share, hidden_units, width), BF16),
        pltpu.VMEM((rows * (query_cols // HEAD_SIZE), key_cols), F32),
        pltpu.VMEM((rows, query_cols), BF16),
        pltpu.VMEM((rows, query_cols * n_tp), BF16),
        pltpu.VMEM((pairs, 2, slice_width), BF16),
        pltpu.VMEM((half, n_tp, pairs, 2, slice_width), BF16),
        pltpu.VMEM((half * ROW_TILE, width), F32),
        pltpu.VMEM((n_tp // share, share, half, pairs, 2, slice_width), BF16),
        pltpu.VMEM((n_messages, pairs, 2, slice_width), BF16),
        pltpu.SemaphoreType.DMA((10,)),
        pltpu.SemaphoreType.DMA((2,)),
        pltpu.SemaphoreType.DMA((3,)),
        pltpu.SemaphoreType.DMA((5,)),
        pltpu.SemaphoreType.DMA((5,)),
    ]
    results = pl.pallas_call(
        functools.partial(layer_kernel, n_ep, n_tp, n_messages),
        out_shape=(
            pltpu.VMEM((rows, slice_width), BF16),
            pltpu.VMEM((rows, key_cols), BF16),
            pltpu.VMEM((rows, key_cols), BF16),
        ),
        in_specs=[pl.BlockSpec(memory_space=pltpu.HBM)] * len(operands),
        out_specs=tuple([pl.BlockSpec(memory_space=pltpu.VMEM)] * 3),
        scratch_shapes=scratch,
        compiler_params=pltpu.CompilerParams(
            collective_id=0, has_side_effects=True, vmem_limit_bytes=66990080
        ),
        name="layer",
    )(*operands)
    return pl.pallas_call(
        place_results,
        out_shape=tuple(jax.ShapeDtypeStruct(r.shape, r.dtype) for r in results),
        in_specs=[pl.BlockSpec(memory_space=pltpu.VMEM)] * 3,
        out_specs=tuple([pl.BlockSpec(memory_space=pltpu.HBM)] * 3),
        scratch_shapes=[pltpu.SemaphoreType.DMA((3,))],
        compiler_params=pltpu.CompilerParams(vmem_limit_bytes=2**20),
        name="place",
    )(*results)


def solution(mesh):
    in_specs = (
        P(("grp", "ep"), None),
        P(),
        P(None, "tp"),
        P(None, "tp"),
        P(None, "tp"),
        P(("grp", "ep"), "tp", None),
        P(("grp", "ep"), "tp", None),
        P(("grp", "ep")),
        P("tp"),
        P(None, "tp"),
        P(),
        P(("grp", "ep"), None),
        P(("grp", "ep"), None),
        P("ep", None, "tp"),
        P("ep", None, "tp"),
        P("ep", "tp", None),
    )
    out_specs = (P(("grp", "ep"), "tp"), P(("grp", "ep"), "tp"), P(("grp", "ep"), "tp"))
    return jax.shard_map(shards, mesh=mesh, in_specs=in_specs, out_specs=out_specs, check_vma=False)
```

```python
import functools

import jax
import jax.numpy as jnp
from jax import lax
from jax.experimental import pallas as pl
from jax.experimental.pallas import tpu as pltpu
from jax.sharding import PartitionSpec as P

HEAD_SIZE = 64
EPSILON = 1e-06
ROW_TILE = 16
MESH_IDS = pl.DeviceIdType.MESH
F32 = jnp.float32
BF16 = jnp.bfloat16


def iota(shape, dim):
    return lax.broadcasted_iota(jnp.int32, shape, dim)


def dot(a, b):
    return jnp.dot(a, b, preferred_element_type=F32)


def layer_kernel(
    n_ep,
    n_tp,
    n_messages,
    tokens_hbm,
    attn_gain_hbm,
    w_query_hbm,
    w_key_hbm,
    w_value_hbm,
    key_hbm,
    value_hbm,
    lengths_hbm,
    head_bias_hbm,
    w_out_hbm,
    ffn_gain_hbm,
    route_ids_hbm,
    route_weights_hbm,
    w_gate_hbm,
    w_up_hbm,
    w_down_hbm,
    mixed_ref,
    new_keys_ref,
    new_values_ref,
    tokens,
    attn_gain,
    w_query,
    w_key,
    w_value,
    keys,
    values,
    lengths,
    head_bias,
    w_out,
    ffn_gain,
    route_ids,
    route_weights,
    w_in,
    w_down,
    spread,
    heads_near,
    heads_far,
    head_rows,
    near_hidden,
    partial_acts,
    hidden_part,
    hidden_near,
    hidden_far,
    hidden_rows,
    out_parts,
    returned,
    small_sem,
    pair_sem,
    weight_sem,
    send_sem,
    recv_sem,
):
    ep = lax.axis_index("ep")
    tp = lax.axis_index("tp")
    rows = tokens.shape[0]
    query_cols = w_query.shape[1]
    key_cols = w_key_hbm.shape[1]
    heads = query_cols // HEAD_SIZE
    group = query_cols // key_cols
    slice_width = w_out.shape[1]
    cache_len = keys.shape[2]
    pairs = rows // 2

    def far_ep(step):
        from_top = jnp.where(n_ep - 1 - step > ep, n_ep - 1 - step, n_ep - 2 - step)
        from_bottom = jnp.where(step < ep, step, step + 1)
        return jnp.where(2 * ep < n_ep, from_top, from_bottom)

    def other_tp(step):
        chip = lax.rem(tp // 2 + 1 + step // 2, n_tp // 2)
        return chip * 2 + lax.rem(tp + step, 2)

    tp_order = [other_tp(step) for step in range(n_tp - 2)]
    tp_order += [other_tp(n_tp - 1), tp]

    share = n_ep * n_tp // n_messages
    half, chips = n_ep // share, n_tp // share
    side, chip, keeper = lax.rem(tp, share), tp // share, share - 1 - ep // half
    first_ep = (share - 1 - side) * half
    mine = keeper == side
    other_chips = [lax.rem(chip + 1 + step, chips) for step in range(chips - 1)]

    def copy_to(source, target, number, peer_ep, peer_tp):
        pltpu.make_async_remote_copy(
            src_ref=source,
            dst_ref=target,
            send_sem=send_sem.at[number],
            recv_sem=recv_sem.at[number],
            device_id={"ep": peer_ep, "tp": peer_tp},
            device_id_type=MESH_IDS,
        ).start()

    def repeat(count, fn):
        if count <= 4:
            for step in range(count):
                fn(step)
        else:
            pl.loop(0, count)(fn)

    barrier = pltpu.get_barrier_semaphore()

    def greet(peer_ep, peer_tp):
        pl.semaphore_signal(
            barrier,
            inc=1,
            device_id={"ep": peer_ep, "tp": peer_tp},
            device_id_type=MESH_IDS,
        )

    def load(source, target, sem):
        copy = pltpu.make_async_copy(source, target, sem)
        copy.start()
        return copy

    token_load = load(tokens_hbm, tokens, small_sem.at[0])
    gain_load = load(attn_gain_hbm, attn_gain, small_sem.at[1])
    query_load = load(w_query_hbm, w_query, small_sem.at[2])
    def load_cache(source, target, sem):
        for pair in range(pairs):
            part = pl.ds(2 * pair, 2)
            pltpu.make_async_copy(source.at[part], target.at[part], sem).start()
        return pltpu.make_async_copy(target, target, sem)

    key_load = load_cache(key_hbm, keys, pair_sem.at[0])
    for step in range(n_ep - 1):
        greet(far_ep(step), tp)
    for peer_tp in tp_order[:-1]:
        greet(ep, peer_tp)
    value_load = load_cache(value_hbm, values, pair_sem.at[1])
    length_load = load(lengths_hbm, lengths, small_sem.at[3])
    bias_load = load(head_bias_hbm, head_bias, small_sem.at[4])
    hidden_rows[...] = jnp.zeros_like(hidden_rows)

    block_len = 256 if cache_len % 256 == 0 else 128
    n_blocks = cache_len // block_len
    triangle = (
        iota((block_len, block_len), 0) > iota((block_len, block_len), 1)
    ).astype(BF16)
    flat = rows * heads
    seq_col = lax.rem(iota((flat, 1), 0), rows)
    head_col = iota((flat, 1), 0) // rows

    token_load.wait()
    rows_f32 = tokens[...].astype(F32)
    gain_load.wait()
    normed = (
        rows_f32
        * lax.rsqrt(jnp.mean(rows_f32 * rows_f32, axis=1, keepdims=True) + EPSILON)
        * attn_gain[...]
    ).astype(BF16)
    query_load.wait()
    for number, source in enumerate((w_gate_hbm, w_up_hbm)):
        pltpu.make_async_copy(source.at[0], w_in.at[0, number], weight_sem.at[1]).start()
    weight_loads = [
        pltpu.make_async_copy(w_in.at[0], w_in.at[0], weight_sem.at[1]),
        load(w_down_hbm.at[0], w_down.at[0], weight_sem.at[2]),
    ]
    own_loads = [
        load(w_key_hbm, w_key, small_sem.at[5]),
        load(w_value_hbm, w_value, small_sem.at[9]),
    ]
    out_load = load(w_out_hbm, w_out, weight_sem.at[0])
    route_loads = [
        load(ffn_gain_hbm, ffn_gain, small_sem.at[6]),
        load(route_ids_hbm, route_ids, small_sem.at[7]),
        load(route_weights_hbm, route_weights, small_sem.at[8]),
    ]
    queries = dot(normed, w_query[...]).astype(BF16).astype(F32)
    for head in range(heads):
        first = head // group * HEAD_SIZE
        piece = queries[:, head * HEAD_SIZE : (head + 1) * HEAD_SIZE]
        sides = [jnp.zeros((rows, first), F32)] if first else []
        sides.append(piece)
        if key_cols > first + HEAD_SIZE:
            sides.append(jnp.zeros((rows, key_cols - first - HEAD_SIZE), F32))
        spread[head * rows : (head + 1) * rows, :] = jnp.concatenate(sides, axis=1)
    folded = spread[...].astype(BF16)
    query_block = jnp.where(
        iota((flat, rows * key_cols), 1) // key_cols == seq_col,
        jnp.concatenate([folded] * rows, axis=1),
        0.0,
    ).astype(BF16)

    length_load.wait()
    bias_load.wait()
    length_col = jnp.zeros((flat, 1), jnp.int32)
    for row in range(rows):
        length_col = jnp.where(seq_col == row, lengths[row], length_col)
    bias_col = jnp.zeros((flat, 1), F32)
    for head in range(heads):
        bias_col = jnp.where(head_col == head, head_bias[head], bias_col)

    key_load.wait()
    key_rows = keys[...].reshape(rows * key_cols, cache_len)
    scores = dot(query_block, key_rows) * HEAD_SIZE ** (-0.5) + bias_col
    in_cache = iota((flat, cache_len), 1) < length_col
    soft = jnp.log(1.0 + jnp.exp(-jnp.abs(scores)))
    log_rest = jnp.where(in_cache, jnp.minimum(-scores, 0.0) - soft, 0.0)
    log_take = jnp.minimum(scores, 0.0) - soft
    high = log_rest.astype(BF16)
    low = (log_rest - high.astype(F32)).astype(BF16)
    stacked = jnp.concatenate(
        [
            part[:, block * block_len : (block + 1) * block_len]
            for part in (high, low)
            for block in range(n_blocks)
        ],
        axis=0,
    )
    within = dot(stacked, triangle)
    carried = jnp.zeros((flat, 1), F32)
    tails = [None] * n_blocks
    for block in reversed(range(n_blocks)):
        tails[block] = (
            within[block * flat : (block + 1) * flat]
            + within[(n_blocks + block) * flat : (n_blocks + block + 1) * flat]
            + carried
        )
        part = log_rest[:, block * block_len : (block + 1) * block_len]
        carried = carried + jnp.sum(part, axis=1, keepdims=True)
    tail_sum = jnp.concatenate(tails, axis=1)
    breaks = jnp.where(in_cache, jnp.exp(log_take + tail_sum), 0.0).astype(BF16)
    value_load.wait()
    value_rows = values[...].reshape(rows * key_cols, cache_len)
    crossed = lax.dot_general(
        breaks, value_rows, (((1,), (1,)), ((), ())), preferred_element_type=F32
    )
    own = jnp.zeros((flat, key_cols), F32)
    for row in range(rows):
        own = jnp.where(seq_col == row, crossed[:, row * key_cols : (row + 1) * key_cols], own)
    spread[...] = own
    key_lane = iota((rows, key_cols), 1) // HEAD_SIZE
    tiles = []
    for place in range(group):
        tile = spread[place * rows : (place + 1) * rows, :]
        for key_head in range(1, heads // group):
            head = key_head * group + place
            tile = jnp.where(key_lane == key_head, spread[head * rows : (head + 1) * rows, :], tile)
        tiles.append(tile)
    heads_out = jnp.concatenate(tiles, axis=1).astype(BF16)

    pl.semaphore_wait(barrier, n_ep + n_tp - 2)
    def put_pairs(target, value):
        for pair in range(pairs):
            target[pair] = value[2 * pair : 2 * pair + 2]

    def chip_heads(parts):
        for member in range(share):
            for pair in range(pairs):
                head_rows[
                    2 * pair : 2 * pair + 2, member * query_cols : (member + 1) * query_cols
                ] = parts[member, pair].astype(F32)
        return head_rows[...].astype(BF16)

    def chip_projection(parts, peer_chip):
        first = pl.multiple_of(peer_chip * share * query_cols, HEAD_SIZE)
        out_rows = [
            w_out[pl.ds(first + offset, HEAD_SIZE), :]
            for start in range(0, share * query_cols, query_cols)
            for place in range(group)
            for offset in range(start + place * HEAD_SIZE, start + query_cols, group * HEAD_SIZE)
        ]
        return dot(chip_heads(parts), jnp.concatenate(out_rows, axis=0))

    head_part = heads_near.at[side]
    put_pairs(head_part, heads_out)
    for step, peer_chip in enumerate(other_chips):
        for member in range(share):
            target = heads_far.at[chips - 2 - step, side]
            copy_to(head_part, target, 5, ep, peer_chip * share + member)
    partner = tp + 1 - 2 * side
    if share == 2:
        copy_to(head_part, head_part, 0, ep, partner)
    weight_loads[0].wait()
    if share == 2:
        copy_to(w_in.at[0], w_in.at[1], 3, ep, partner)
    for copy in own_loads:
        copy.wait()
    new_keys_ref[...] = dot(normed, w_key[...]).astype(BF16)
    new_values_ref[...] = dot(normed, w_value[...]).astype(BF16)
    out_load.wait()
    slice_cols = pl.ds(pl.multiple_of(tp * slice_width, slice_width), slice_width)
    own_hidden = tokens[:, slice_cols].astype(F32)
    if share == 2:
        pltpu.make_async_copy(head_part, head_part, recv_sem.at[0]).wait()
    near_hidden[...] = own_hidden + chip_projection(heads_near, chip)
    pltpu.make_async_copy(heads_far, heads_far, recv_sem.at[5]).wait()
    own_hidden = near_hidden[...]
    for step, peer_chip in enumerate(other_chips):
        own_hidden = own_hidden + chip_projection(heads_far.at[step], peer_chip)

    put_pairs(hidden_part, own_hidden.astype(BF16))
    row_slot = lax.rem(ep, half)
    near_slot = hidden_near.at[row_slot, side]

    def send_hidden(peer_ep):
        for step, peer_chip in enumerate(other_chips):
            target = hidden_far.at[chips - 2 - step, row_slot, side]
            copy_to(hidden_part, target, 6, peer_ep, peer_chip * share + keeper)

    def send_hidden_far(step):
        send_hidden(far_ep(step))
        copy_to(hidden_part, near_slot, 1, far_ep(step), chip * share + keeper)

    repeat(n_ep - 1, send_hidden_far)
    send_hidden(ep)

    @pl.when(mine)
    def _():
        pltpu.make_async_copy(hidden_part, near_slot, recv_sem.at[1]).start()

    if share == 2:

        @pl.when(jnp.logical_not(mine))
        def _():
            copy_to(hidden_part, near_slot, 1, ep, partner)

    weight_loads[1].wait()
    if share == 2:
        copy_to(w_down.at[0], w_down.at[1], 4, ep, partner)
    for copy in route_loads:
        copy.wait()
    diagonal = iota((rows, rows), 0) == iota((rows, rows), 1)
    choices = []
    for choice in range(route_ids.shape[0]):
        id_row = route_ids[choice : choice + 1, :].astype(F32)
        weight_row = route_weights[choice : choice + 1, :]
        choices.append(
            tuple(
                jnp.sum(jnp.where(diagonal, row, 0.0), axis=1, keepdims=True)
                for row in (id_row, weight_row)
            )
        )
    if share == 2:
        pltpu.make_async_copy(w_in.at[1], w_in.at[1], recv_sem.at[3]).wait()
    chip_width = share * slice_width

    def chip_rows(parts, target, peer_chip):
        for source in range(half):
            for member in range(share):
                part = slice(member * slice_width, (member + 1) * slice_width)
                for pair in range(pairs):
                    first = source * ROW_TILE + 2 * pair
                    target[first : first + 2, part] = parts[source, member, pair].astype(F32)
        hidden = target[...]
        cols = pl.ds(pl.multiple_of(peer_chip * chip_width, chip_width), chip_width)
        scaled = (hidden * ffn_gain[:, cols]).astype(BF16)
        terms = [
            dot(scaled, w_in[member, kind, cols, :])
            for member in range(share)
            for kind in range(2)
        ]
        return jnp.sum(hidden * hidden, axis=1, keepdims=True), terms

    pltpu.make_async_copy(hidden_near, hidden_near, recv_sem.at[1]).wait()
    squares, near_terms = chip_rows(hidden_near, hidden_rows.at[0], chip)
    for number, term in enumerate(near_terms):
        partial_acts[number] = term
    pltpu.make_async_copy(hidden_far, hidden_far, recv_sem.at[6]).wait()
    terms = [partial_acts[number] for number in range(2 * share)]
    for step, peer_chip in enumerate(other_chips):
        more, others = chip_rows(hidden_far.at[step], hidden_rows.at[step + 1], peer_chip)
        squares = squares + more
        terms = [term + other for term, other in zip(terms, others)]
    row_scale = lax.rsqrt(squares * (1.0 / (n_tp * slice_width)) + EPSILON)
    acts = []
    for member in range(share):
        gate_act = terms[2 * member] * row_scale
        up_act = terms[2 * member + 1] * row_scale
        acts.append((gate_act / (1.0 + jnp.exp(-gate_act)) * up_act).astype(BF16))
    hidden_act = jnp.concatenate(acts, axis=1)
    if share == 2:
        pltpu.make_async_copy(w_down.at[1], w_down.at[1], recv_sem.at[4]).wait()
    out_slot = returned.at[ep * chips + chip]
    for order, peer_chip in enumerate(other_chips + [chip]):
        cols = pl.ds(pl.multiple_of(peer_chip * chip_width, chip_width), chip_width)
        down = w_down[:, :, cols].reshape(hidden_act.shape[1], chip_width)
        expert_rows = dot(hidden_act, down).astype(BF16)
        for source in range(half):
            for member in range(share):
                part = slice(member * slice_width, (member + 1) * slice_width)
                for pair in range(pairs):
                    first = source * ROW_TILE + 2 * pair
                    out_parts[order, member, source, pair] = expert_rows[first : first + 2, part]

        def send_out(step):
            source = jnp.where(2 * ep >= 2 * first_ep + half, step, half - 1 - step)
            owner = first_ep + source
            if order < chips - 1:
                for member in range(share):
                    peer_tp = peer_chip * share + member
                    copy_to(out_parts.at[order, member, source], out_slot, 2, owner, peer_tp)
                return
            if share == 2:
                copy_to(out_parts.at[order, 1 - side, source], out_slot, 2, owner, partner)

            @pl.when(owner != ep)
            def _():
                copy_to(out_parts.at[order, side, source], out_slot, 2, owner, tp)

            @pl.when(owner == ep)
            def _():
                pltpu.make_async_copy(
                    out_parts.at[order, side, source], out_slot, recv_sem.at[2]
                ).start()

        repeat(half, send_out)
    pltpu.make_async_copy(returned, returned, recv_sem.at[2]).wait()

    def expert_part(number):
        return jnp.concatenate(
            [returned[number, pair].astype(F32) for pair in range(pairs)], axis=0
        )

    mixed = own_hidden
    for expert in range(n_ep):
        total = expert_part(expert * chips)
        for number in range(1, chips):
            total = total + expert_part(expert * chips + number)
        scale = jnp.zeros((rows, 1), F32)
        for id_col, weight_col in choices:
            scale = scale + jnp.where(id_col == expert, weight_col, 0.0)
        mixed = mixed + scale * total.astype(BF16).astype(F32)
    mixed_ref[...] = mixed.astype(BF16)

    pltpu.make_async_copy(heads_far, heads_far, send_sem.at[5]).wait()
    if share == 2:
        pltpu.make_async_copy(head_part, head_part, send_sem.at[0]).wait()
    sent_far = returned.at[pl.ds(0, n_ep * (chips - 1))]
    pltpu.make_async_copy(sent_far, sent_far, send_sem.at[6]).wait()
    for number, most in ((1, n_ep), (2, n_messages)):

        @pl.when(mine)
        def _():
            sent = returned.at[pl.ds(0, most - 1)]
            pltpu.make_async_copy(sent, sent, send_sem.at[number]).wait()

        @pl.when(jnp.logical_not(mine))
        def _():
            sent = returned.at[pl.ds(0, most)]
            pltpu.make_async_copy(sent, sent, send_sem.at[number]).wait()

    if share == 2:
        pltpu.make_async_copy(w_in.at[1], w_in.at[1], send_sem.at[3]).wait()
        pltpu.make_async_copy(w_down.at[1], w_down.at[1], send_sem.at[4]).wait()


def place_results(*refs):
    copies = [
        pltpu.make_async_copy(refs[number], refs[3 + number], refs[6].at[number])
        for number in range(3)
    ]
    for copy in copies:
        copy.start()
    for copy in copies:
        copy.wait()


def shards(
    tokens,
    attn_gain,
    w_query,
    w_key,
    w_value,
    key_cache,
    value_cache,
    lengths,
    head_bias,
    w_out,
    ffn_gain,
    route_ids,
    route_weights,
    w_gate,
    w_up,
    w_down,
):
    n_ep = lax.axis_size("ep")
    n_tp = lax.axis_size("tp")
    rows, width = tokens.shape
    query_cols = w_query.shape[1]
    key_cols = w_key.shape[1]
    slice_width = w_out.shape[1]
    operands = (
        tokens,
        attn_gain.reshape(1, width),
        w_query,
        w_key,
        w_value,
        key_cache,
        value_cache,
        lengths,
        head_bias,
        w_out,
        ffn_gain.reshape(1, width),
        route_ids.T,
        route_weights.T,
        w_gate,
        w_up,
        w_down,
    )
    in_smem = (7, 8)
    buffers = [
        (pltpu.SMEM if number in in_smem else pltpu.VMEM)(operand.shape, operand.dtype)
        for number, operand in enumerate(operands[:13])
    ]
    share = 2 if n_ep % 2 == 0 and n_tp % 2 == 0 else 1
    half, chips, pairs = n_ep // share, n_tp // share, rows // 2
    n_messages = half * n_tp
    hidden_units = w_gate.shape[2]
    scratch = buffers + [
        pltpu.VMEM((share, 2, width, hidden_units), BF16),
        pltpu.VMEM((share, hidden_units, width), BF16),
        pltpu.VMEM((rows * (query_cols // HEAD_SIZE), key_cols), F32),
        pltpu.VMEM((share, pairs, 2, query_cols), BF16),
        pltpu.VMEM((chips - 1, share, pairs, 2, query_cols), BF16),
        pltpu.VMEM((rows, share * query_cols), F32),
        pltpu.VMEM((rows, slice_width), F32),
        pltpu.VMEM((2 * share, half * ROW_TILE, hidden_units), F32),
        pltpu.VMEM((pairs, 2, slice_width), BF16),
        pltpu.VMEM((half, share, pairs, 2, slice_width), BF16),
        pltpu.VMEM((chips - 1, half, share, pairs, 2, slice_width), BF16),
        pltpu.VMEM((chips, half * ROW_TILE, share * slice_width), F32),
        pltpu.VMEM((chips, share, half, pairs, 2, slice_width), BF16),
        pltpu.VMEM((n_messages, pairs, 2, slice_width), BF16),
        pltpu.SemaphoreType.DMA((10,)),
        pltpu.SemaphoreType.DMA((2,)),
        pltpu.SemaphoreType.DMA((3,)),
        pltpu.SemaphoreType.DMA((7,)),
        pltpu.SemaphoreType.DMA((7,)),
    ]
    results = pl.pallas_call(
        functools.partial(layer_kernel, n_ep, n_tp, n_messages),
        out_shape=(
            pltpu.VMEM((rows, slice_width), BF16),
            pltpu.VMEM((rows, key_cols), BF16),
            pltpu.VMEM((rows, key_cols), BF16),
        ),
        in_specs=[pl.BlockSpec(memory_space=pltpu.HBM)] * len(operands),
        out_specs=tuple([pl.BlockSpec(memory_space=pltpu.VMEM)] * 3),
        scratch_shapes=scratch,
        compiler_params=pltpu.CompilerParams(
            collective_id=0, has_side_effects=True, vmem_limit_bytes=66990080
        ),
        name="layer",
    )(*operands)
    return pl.pallas_call(
        place_results,
        out_shape=tuple(jax.ShapeDtypeStruct(r.shape, r.dtype) for r in results),
        in_specs=[pl.BlockSpec(memory_space=pltpu.VMEM)] * 3,
        out_specs=tuple([pl.BlockSpec(memory_space=pltpu.HBM)] * 3),
        scratch_shapes=[pltpu.SemaphoreType.DMA((3,))],
        compiler_params=pltpu.CompilerParams(vmem_limit_bytes=2**20),
        name="place",
    )(*results)


def solution(mesh):
    in_specs = (
        P(("grp", "ep"), None),
        P(),
        P(None, "tp"),
        P(None, "tp"),
        P(None, "tp"),
        P(("grp", "ep"), "tp", None),
        P(("grp", "ep"), "tp", None),
        P(("grp", "ep")),
        P("tp"),
        P(None, "tp"),
        P(),
        P(("grp", "ep"), None),
        P(("grp", "ep"), None),
        P("ep", None, "tp"),
        P("ep", None, "tp"),
        P("ep", "tp", None),
    )
    out_specs = (P(("grp", "ep"), "tp"), P(("grp", "ep"), "tp"), P(("grp", "ep"), "tp"))
    return jax.shard_map(shards, mesh=mesh, in_specs=in_specs, out_specs=out_specs, check_vma=False)
```
